32 devices in a mesh: sp: 8 (over z, y), tp: 4 (over x, core).
Axes of the slice: x: 2, y: 2, z: 4, core: 2. Of those that a mesh axis runs over, the one named last changes fastest.
Arguments:
- prompt_input: bfloat16 [2304, 2048], P('sp'), may hold values from -6 to 6
- next_input: bfloat16 [2048], replicated, may hold values from -6 to 6
- norm_gain: float32 [2048], replicated, may hold values from 0.1 to 1.9
- w_key: bfloat16 [2048, 1024], P(None, 'tp'), may hold values from -0.125 to 0.125
- w_value: bfloat16 [2048, 1024], P(None, 'tp'), may hold values from -0.125 to 0.125
- w_query: bfloat16 [2048, 1024], P(None, 'tp'), may hold values from -0.125 to 0.125
- key_offset: float32 [2304, 8], P('sp', 'tp'), may hold values from -10 to 0, as said below
Outputs:
- key_cache: bfloat16 [8, 8, 36, 1024], P('sp', None, None, 'tp')
- value_cache: bfloat16 [8, 8, 36, 1024], P('sp', None, None, 'tp')
- reading: bfloat16 [1024], replicated
The draws below stay inside these ranges and needn't reach their ends.
Inputs may be any that keep to these rules, and one draw needn't show every extreme that they name: `key_offset`: finite log-odds offsets, one per key and head.
All inputs are finite; a program needn't handle non-finite values.
Results may differ from the reference program's by a relative error of at most 0.011.
Values may be sent and summed in bfloat16 or wider, within the bound.
A program may use at most 64 MiB of HBM per device.

```python
import math
import jax
import jax.numpy as jnp
from jax import lax

D = 2048
HEAD_COUNT = 8
HEAD_DIM = 128
SPAN = 288
PROMPT_LENGTH = 2304
SUB = 36
N_SP = 8


def draw_key_offset(key, part):
    head_order = jax.random.permutation(jax.random.fold_in(key, 11), HEAD_COUNT)
    fast_heads = head_order < HEAD_COUNT // 2
    slow_base = math.log(0.6 / PROMPT_LENGTH)
    fast_base = math.log(0.6 / 40.0)
    base_rate = jnp.where(fast_heads, fast_base, slow_base).astype(jnp.float32)
    block_shift = jax.random.uniform(jax.random.fold_in(key, 12), (HEAD_COUNT, PROMPT_LENGTH // SPAN), jnp.float32, -0.7, 0.7)
    block_shift = jnp.repeat(block_shift, SPAN, axis=1)
    rough_part = jax.random.uniform(jax.random.fold_in(key, 13), (HEAD_COUNT, PROMPT_LENGTH), jnp.float32, -1.0, 1.0)
    offset_table = base_rate[:, None] + block_shift + rough_part
    spike_position = jax.random.randint(jax.random.fold_in(key, 14), (HEAD_COUNT, 3), 0, PROMPT_LENGTH)
    position_slots = jnp.arange(PROMPT_LENGTH, dtype=jnp.int32)
    spike_matches = jnp.any(position_slots[None, None, :] == spike_position[..., None], axis=1)
    signal_level = jax.random.uniform(jax.random.fold_in(key, 15), (HEAD_COUNT, PROMPT_LENGTH), jnp.float32, -1.4, 0.0)
    gradual_mask = jnp.logical_not(fast_heads)[:, None]
    offset_table = jnp.where(jnp.logical_and(spike_matches, gradual_mask), signal_level, offset_table)
    offset_table = jnp.clip(offset_table, -10.0, 0.0)
    return jnp.transpose(offset_table, (1, 0)).astype(jnp.float32)


def steps_of(rng, shape, cuts, least, largest):
    level = 1.0
    for position, parts in cuts:
        steps = jax.random.uniform(jax.random.fold_in(jax.random.fold_in(rng, 6), position), (parts,), jnp.float32, least / len(cuts), largest / len(cuts))
        level = level * jnp.repeat(jnp.exp(steps), shape[position] // parts).reshape((-1,) + (1,) * (len(shape) - 1 - position))
    return level


def noise(key, extent, deviation, most, shards=(), held_as=jnp.bfloat16):
    drawn = deviation * jax.random.normal(key, extent, jnp.float32)
    if shards:
        drawn = drawn * steps_of(key, extent, shards, -0.22, 0.18)
    return jnp.clip(drawn, -most, most).astype(held_as)


def setup_inputs(seed: int = 0) -> dict:
    streams_of = jax.random.split(jax.random.key(seed), 8)
    return {
        "prompt_input": noise(streams_of[0], (PROMPT_LENGTH, D), 1.0, 6.0, ((0, 8),)),
        "next_input": noise(streams_of[1], (D,), 1.0, 6.0),
        "norm_gain": jnp.clip(1.0 + 0.18 * jax.random.normal(streams_of[2], (D,), jnp.float32), 0.1, 1.9),
        "w_key": noise(streams_of[3], (D, HEAD_COUNT * HEAD_DIM), D ** -0.5, 0.125, ((1, 4),)),
        "w_value": noise(streams_of[4], (D, HEAD_COUNT * HEAD_DIM), D ** -0.5, 0.125, ((1, 4),)),
        "w_query": noise(streams_of[5], (D, HEAD_COUNT * HEAD_DIM), D ** -0.5, 0.125, ((1, 4),)),
        "key_offset": draw_key_offset(jax.random.fold_in(streams_of[7], 71), 0),
    }


def norm_rows(row_block, gain_vec):
    wide_rows = row_block.astype(jnp.float32)
    inv_rms = lax.rsqrt(lax.optimization_barrier(jnp.mean(wide_rows * wide_rows, axis=-1, keepdims=True)) + 1e-06)
    return (wide_rows * inv_rms * gain_vec).astype(jnp.bfloat16)

def lay_out(cache_rows):
    blocks = cache_rows.reshape(N_SP, N_SP, SUB, HEAD_COUNT * HEAD_DIM)
    return jnp.transpose(blocks, (1, 0, 2, 3))

def reference(prompt_input, next_input, norm_gain, w_key, w_value, w_query, key_offset):
    normed = norm_rows(prompt_input, norm_gain)
    keys = jnp.dot(normed, w_key, preferred_element_type=jnp.float32).astype(jnp.bfloat16)
    values = jnp.dot(normed, w_value, preferred_element_type=jnp.float32).astype(jnp.bfloat16)
    query_normed = norm_rows(next_input[None, :], norm_gain)
    new_query = jnp.dot(query_normed, w_query, preferred_element_type=jnp.float32).astype(jnp.bfloat16)
    new_query = new_query.reshape(HEAD_COUNT, HEAD_DIM).astype(jnp.float32)
    key_heads = keys.reshape(PROMPT_LENGTH, HEAD_COUNT, HEAD_DIM).astype(jnp.float32)
    value_heads = values.reshape(PROMPT_LENGTH, HEAD_COUNT, HEAD_DIM).astype(jnp.float32)
    logits = jnp.einsum('hd,shd->sh', new_query, key_heads) * HEAD_DIM ** (-0.5) + key_offset
    log_breaks = jax.nn.log_sigmoid(-logits)
    later = lax.cumsum(log_breaks, axis=0, reverse=True) - log_breaks
    weights = jnp.exp(jax.nn.log_sigmoid(logits) + later)
    reading = jnp.einsum('sh,shd->hd', weights, value_heads)
    reading = reading.reshape(HEAD_COUNT * HEAD_DIM).astype(jnp.bfloat16)
    return (lay_out(keys), lay_out(values), reading)
```

```python
import functools

import jax
import jax.numpy as jnp
from jax import lax
from jax.experimental import pallas as pl
from jax.experimental.pallas import tpu as pltpu
from jax.sharding import PartitionSpec as P

HEAD_DIM = 128
MESH = pl.DeviceIdType.MESH


def inverse_rms(wide):
    return lax.rsqrt(jnp.mean(wide * wide, axis=-1, keepdims=True) + 1e-06)


def split_parts(wide, count):
    parts = []
    for _ in range(count):
        part = wide.astype(jnp.bfloat16).astype(jnp.float32)
        parts.append(part)
        wide = wide - part
    return jnp.concatenate(parts, axis=0).astype(jnp.bfloat16)


def fold_parts(rows, heads):
    total = rows[:heads]
    for first in range(heads, rows.shape[0], heads):
        total = total + rows[first : first + heads]
    return total


def pack_blocks(wide, outgoing, landed, me, heads, sub):
    for slot in range(outgoing.shape[0]):
        outgoing[slot] = jnp.concatenate(
            [
                wide[slot * sub : (slot + 1) * sub, head * HEAD_DIM : (head + 1) * HEAD_DIM]
                for head in range(heads)
            ],
            axis=0,
        ).astype(jnp.bfloat16)
    landed[me] = outgoing[me]


def kernel(
    n_sp, n_tp, chunks,
    x_hbm, next_hbm, gain_hbm, wk_hbm, wv_hbm, wq_hbm, offset_hbm,
    k_landed, v_landed, read_out,
    x_in, scaled, inverse, next_in, gain_in, wk, wv, wq, offset, later_than,
    k_outgoing, v_outgoing, message, gathered,
    x_sem, load_sem,
    k_ssem, k_rsem, v_ssem, v_rsem, m_ssem, m_rsem, ready,
):
    me = lax.axis_index("sp")
    lane = lax.axis_index("tp")
    span, width = x_hbm.shape[0], wk_hbm.shape[1]
    heads = width // HEAD_DIM
    sub = span // n_sp
    rows = span // chunks
    unroll = n_sp <= 16

    load_gain, load_next, load_offset, load_key, load_query, load_value = [
        pltpu.make_async_copy(hbm, vmem, load_sem.at[n])
        for n, (hbm, vmem) in enumerate(
            [
                (gain_hbm, gain_in),
                (next_hbm, next_in),
                (offset_hbm, offset),
                (wk_hbm, wk),
                (wq_hbm, wq),
                (wv_hbm, wv),
            ]
        )
    ]
    x_loads = [
        pltpu.make_async_copy(
            x_hbm.at[pl.ds(c * rows, rows)], x_in.at[pl.ds(c * rows, rows)], x_sem.at[c]
        )
        for c in range(chunks)
    ]
    load_gain.start()
    for load in x_loads:
        load.start()
    load_key.start()
    load_next.start()
    load_offset.start()
    load_query.start()
    load_value.start()

    barrier = pltpu.get_barrier_semaphore()

    @pl.loop(1, n_sp)
    def _(step):
        pl.semaphore_signal(
            barrier, inc=1, device_id=(lax.rem(me + step, n_sp), lane), device_id_type=MESH
        )

    @pl.loop(1, n_tp)
    def _(step):
        pl.semaphore_signal(
            barrier, inc=1, device_id=(me, lax.rem(lane + step, n_tp)), device_id_type=MESH
        )

    later_than[...] = jnp.where(
        lax.broadcasted_iota(jnp.int32, (span, span), 0)
        > lax.broadcasted_iota(jnp.int32, (span, span), 1),
        1.0,
        0.0,
    ).astype(jnp.bfloat16)

    load_gain.wait()
    gain = gain_in[...]
    step_rows = 16 if rows % 16 == 0 else rows
    for c in range(chunks):
        x_loads[c].wait()
        for first in range(c * rows, (c + 1) * rows, step_rows):
            wide = x_in[first : first + step_rows, :].astype(jnp.float32)
            scaled[first : first + step_rows, :] = (wide * gain).astype(jnp.bfloat16)
            inverse[first : first + step_rows, :] = jnp.broadcast_to(
                inverse_rms(wide), (step_rows, HEAD_DIM)
            )

    def project(weight):
        wide = jnp.dot(scaled[...], weight[...], preferred_element_type=jnp.float32)
        factor = inverse[...]
        return jnp.concatenate(
            [
                wide[:, head * HEAD_DIM : (head + 1) * HEAD_DIM] * factor
                for head in range(heads)
            ],
            axis=1,
        )

    group = 2 if n_sp % 2 == 0 else 1
    groups = n_sp // group
    mine, place = me // group, lax.rem(me, group)
    upper = mine // ((groups + 1) // 2)

    def partner(order):
        near = order // group
        low = near + jnp.where(near >= mine, 1, 0)
        high = groups - 1 - near
        high = high - jnp.where(high <= mine, 1, 0)
        away = low * upper + high * (1 - upper)
        other = jnp.where(near >= groups - 1, 1, 0)
        chosen = away + other * (mine - away)
        return chosen * group + lax.rem(place + lax.rem(order, group) + other, group)

    def block_copy(outgoing, landed, ssem, rsem, order):
        to = partner(order)
        return pltpu.make_async_remote_copy(
            src_ref=outgoing.at[to], dst_ref=landed.at[me],
            send_sem=ssem.at[order], recv_sem=rsem.at[me],
            device_id=(to, lane), device_id_type=MESH,
        )

    def block_arrival(outgoing, landed, ssem, rsem, step):
        source = lax.rem(me + step, n_sp)
        return pltpu.make_async_remote_copy(
            src_ref=outgoing.at[source], dst_ref=landed.at[source],
            send_sem=ssem.at[step - 1], recv_sem=rsem.at[source],
            device_id=(source, lane), device_id_type=MESH,
        )

    keys_path = (k_outgoing, k_landed, k_ssem, k_rsem)
    values_path = (v_outgoing, v_landed, v_ssem, v_rsem)
    first_sends = group if n_sp > group else 0

    load_key.wait()
    wide_keys = project(wk)
    keys = wide_keys.astype(jnp.bfloat16)
    pack_blocks(wide_keys, k_outgoing, k_landed, me, heads, sub)

    pl.semaphore_wait(barrier, n_sp + n_tp - 2)
    for order in range(first_sends):
        block_copy(*keys_path, order).start()

    @pl.loop(1, n_tp)
    def _(step):
        pl.semaphore_signal(
            ready, inc=1, device_id=(me, lax.rem(lane + step, n_tp)), device_id_type=MESH
        )

    load_value.wait()
    wide_values = project(wv)
    pack_blocks(wide_values, v_outgoing, v_landed, me, heads, sub)
    for order in range(first_sends):
        block_copy(*values_path, order).start()

    load_next.wait()
    load_offset.wait()
    load_query.wait()
    next_row = next_in[...].astype(jnp.float32)
    next_row = jnp.concatenate([next_row[n : n + 1] for n in range(next_row.shape[0])], axis=1)
    next_scaled = jnp.broadcast_to((next_row * gain).astype(jnp.bfloat16), (16, x_hbm.shape[1]))
    query = jnp.dot(next_scaled, wq[...], preferred_element_type=jnp.float32)
    query = query * inverse_rms(next_row)
    row_ids = lax.broadcasted_iota(jnp.int32, query.shape, 0)
    head_ids = lax.broadcasted_iota(jnp.int32, query.shape, 1) // HEAD_DIM
    query = jnp.where(row_ids == head_ids, query, 0.0).astype(jnp.bfloat16)

    logits = lax.dot_general(
        query, keys, (((1,), (1,)), ((), ())), preferred_element_type=jnp.float32
    )[:heads]
    logits = logits * HEAD_DIM ** (-0.5) + offset[...]
    tail = jnp.log1p(jnp.exp(-jnp.abs(logits)))
    log_breaks = -jnp.maximum(logits, 0.0) - tail
    inner = fold_parts(
        jnp.dot(split_parts(log_breaks, 3), later_than[...], preferred_element_type=jnp.float32),
        heads,
    )
    block_total = jnp.sum(log_breaks, axis=1, keepdims=True)
    weights = jnp.exp(jnp.minimum(logits, 0.0) - tail + inner)
    read = fold_parts(
        jnp.dot(
            split_parts(weights, 2),
            wide_values.astype(jnp.bfloat16),
            preferred_element_type=jnp.float32,
        ),
        heads,
    )
    high = block_total.astype(jnp.bfloat16).astype(jnp.float32)
    low = block_total - high
    half = lax.broadcasted_iota(jnp.int32, (heads, HEAD_DIM), 1) < HEAD_DIM // 2
    message[...] = jnp.concatenate(
        [
            read[head : head + 1, head * HEAD_DIM : (head + 1) * HEAD_DIM]
            for head in range(heads)
        ]
        + [jnp.where(half, high, low)],
        axis=0,
    ).astype(jnp.bfloat16)
    gathered[me, lane] = message[...]

    pl.semaphore_wait(ready, n_tp - 1)

    def message_copy(order, step):
        to, to_lane = partner(order), lax.rem(lane + step, n_tp)
        return pltpu.make_async_remote_copy(
            src_ref=message, dst_ref=gathered.at[me, lane],
            send_sem=m_ssem.at[order, step], recv_sem=m_rsem.at[me, lane],
            device_id=(to, to_lane), device_id_type=MESH,
        )

    def own_message_copy(step):
        return pltpu.make_async_remote_copy(
            src_ref=message, dst_ref=gathered.at[me, lane],
            send_sem=m_ssem.at[n_sp - 1, step], recv_sem=m_rsem.at[me, lane],
            device_id=(me, lax.rem(lane + step, n_tp)), device_id_type=MESH,
        )

    def message_arrival(source, step):
        source_lane = lax.rem(lane + step, n_tp)
        return pltpu.make_async_remote_copy(
            src_ref=message, dst_ref=gathered.at[source, source_lane],
            send_sem=m_ssem.at[0, 0], recv_sem=m_rsem.at[source, source_lane],
            device_id=(source, source_lane), device_id_type=MESH,
        )

    @pl.loop(0, n_sp - 1, unroll=unroll)
    def _(order):
        for step in range(n_tp):
            message_copy(order, step).start()

    for step in range(1, n_tp):
        own_message_copy(step).start()

    @pl.loop(first_sends, n_sp - 1, unroll=unroll)
    def _(order):
        block_copy(*keys_path, order).start()
        block_copy(*values_path, order).start()

    for step in range(1, n_tp):
        message_arrival(me, step).wait_recv()

    @pl.loop(1, n_sp)
    def _(step):
        source = lax.rem(me + step, n_sp)
        for lane_step in range(n_tp):
            message_arrival(source, lane_step).wait_recv()

    def add_block(step, carry):
        block = [gathered[n_sp - 1 - step, part].astype(jnp.float32) for part in range(n_tp)]
        fresh = []
        for (total, carried), piece in zip(carry, block):
            total = total + jnp.exp(carried) * piece[:heads]
            halves = piece[heads:]
            fresh.append((total, carried + halves + pltpu.roll(halves, HEAD_DIM // 2, 1)))
        return tuple(fresh)

    zero = jnp.zeros((heads, HEAD_DIM), jnp.float32)
    totals = lax.fori_loop(0, n_sp, add_block, ((zero, zero),) * n_tp, unroll=unroll)
    read_out[...] = jnp.concatenate([total for total, _ in totals], axis=0).astype(jnp.bfloat16)

    for step in range(1, n_tp):
        own_message_copy(step).wait_send()

    @pl.loop(0, n_sp - 1)
    def _(order):
        for step in range(n_tp):
            message_copy(order, step).wait_send()
        block_copy(*keys_path, order).wait_send()
        block_copy(*values_path, order).wait_send()

    @pl.loop(1, n_sp)
    def _(step):
        block_arrival(*keys_path, step).wait_recv()
        block_arrival(*values_path, step).wait_recv()


def finish(k_landed, v_landed, read_in, k_out, v_out, read_out):
    sub, _, width = k_out.shape
    heads = width // HEAD_DIM
    for landed, out in ((k_landed, k_out), (v_landed, v_out)):
        for head in range(heads):
            piece = landed[...].astype(jnp.float32)[:, head * sub : (head + 1) * sub, :]
            out[:, :, head * HEAD_DIM : (head + 1) * HEAD_DIM] = jnp.swapaxes(
                piece, 0, 1
            ).astype(jnp.bfloat16)
    read_out[...] = read_in[...]


def shards(prompt_input, next_input, norm_gain, w_key, w_value, w_query, key_offset):
    span, depth = prompt_input.shape
    width = w_key.shape[1]
    heads = width // HEAD_DIM
    n_sp, n_tp = lax.axis_size("sp"), lax.axis_size("tp")
    sub = span // n_sp
    chunks = 3 if span % 48 == 0 else 1
    wide, narrow = jnp.float32, jnp.bfloat16
    blocks = (n_sp, heads * sub, HEAD_DIM)
    sems = pltpu.SemaphoreType.DMA
    landed = pl.pallas_call(
        functools.partial(kernel, n_sp, n_tp, chunks),
        out_shape=(
            jax.ShapeDtypeStruct(blocks, narrow),
            jax.ShapeDtypeStruct(blocks, narrow),
            jax.ShapeDtypeStruct((n_tp * heads, HEAD_DIM), narrow),
        ),
        in_specs=[pl.BlockSpec(memory_space=pltpu.HBM)] * 7,
        out_specs=(pl.BlockSpec(memory_space=pltpu.VMEM),) * 3,
        scratch_shapes=[
            pltpu.VMEM((span, depth), narrow),
            pltpu.VMEM((span, depth), narrow),
            pltpu.VMEM((span, HEAD_DIM), wide),
            pltpu.VMEM((depth // HEAD_DIM, HEAD_DIM), narrow),
            pltpu.VMEM((1, depth), wide),
            pltpu.VMEM((depth, width), narrow),
            pltpu.VMEM((depth, width), narrow),
            pltpu.VMEM((depth, width), narrow),
            pltpu.VMEM((heads, span), wide),
            pltpu.VMEM((span, span), narrow),
            pltpu.VMEM(blocks, narrow),
            pltpu.VMEM(blocks, narrow),
            pltpu.VMEM((2 * heads, HEAD_DIM), narrow),
            pltpu.VMEM((n_sp, n_tp, 2 * heads, HEAD_DIM), narrow),
            sems((chunks,)),
            sems((6,)),
            sems((n_sp,)),
            sems((n_sp,)),
            sems((n_sp,)),
            sems((n_sp,)),
            sems((n_sp, n_tp)),
            sems((n_sp, n_tp)),
            pltpu.SemaphoreType.REGULAR,
        ],
        compiler_params=pltpu.CompilerParams(
            collective_id=0, has_side_effects=True, vmem_limit_bytes=16 * 2**20
        ),
        name="prefill",
    )(
        *[
            pltpu.with_memory_space_constraint(operand, pltpu.HBM)
            for operand in (
                prompt_input,
                next_input.reshape(-1, HEAD_DIM),
                norm_gain[None],
                w_key,
                w_value,
                w_query,
                key_offset.T,
            )
        ]
    )
    slotted = jax.ShapeDtypeStruct((sub, n_sp, width), narrow)
    key_cache, value_cache, reading = pl.pallas_call(
        finish,
        out_shape=(slotted, slotted, jax.ShapeDtypeStruct((n_tp * heads, HEAD_DIM), narrow)),
        in_specs=[pl.BlockSpec(memory_space=pltpu.VMEM)] * 3,
        out_specs=(pl.BlockSpec(memory_space=pltpu.VMEM),) * 3,
        compiler_params=pltpu.CompilerParams(vmem_limit_bytes=16 * 2**20),
        name="finish",
    )(*landed)
    return (
        jnp.swapaxes(key_cache, 0, 1)[None],
        jnp.swapaxes(value_cache, 0, 1)[None],
        reading.reshape(-1),
    )


def solution(mesh):
    placed = (P("sp", None), P(), P(), P(None, "tp"), P(None, "tp"), P(None, "tp"), P("sp", "tp"))
    return jax.shard_map(
        shards,
        mesh=mesh,
        in_specs=placed,
        out_specs=(P("sp", None, None, "tp"), P("sp", None, None, "tp"), P()),
        check_vma=False,
    )
```

```python
import functools

import jax
import jax.numpy as jnp
from jax import lax
from jax.experimental import pallas as pl
from jax.experimental.pallas import tpu as pltpu
from jax.sharding import PartitionSpec as P

HEAD_DIM = 128
MESH = pl.DeviceIdType.MESH


def inverse_rms(wide):
    return lax.rsqrt(jnp.mean(wide * wide, axis=-1, keepdims=True) + 1e-06)


def split_parts(wide, count):
    parts = []
    for _ in range(count):
        part = wide.astype(jnp.bfloat16).astype(jnp.float32)
        parts.append(part)
        wide = wide - part
    return jnp.concatenate(parts, axis=0).astype(jnp.bfloat16)


def fold_parts(rows, heads):
    total = rows[:heads]
    for first in range(heads, rows.shape[0], heads):
        total = total + rows[first : first + heads]
    return total


def pack_blocks(wide, outgoing, first, heads, sub):
    for slot in range(wide.shape[0] // sub):
        outgoing[first + slot] = jnp.concatenate(
            [
                wide[slot * sub : (slot + 1) * sub, head * HEAD_DIM : (head + 1) * HEAD_DIM]
                for head in range(heads)
            ],
            axis=0,
        ).astype(jnp.bfloat16)


def kernel(
    n_sp, n_tp, chunks,
    x_hbm, next_hbm, gain_hbm, wk_hbm, wv_hbm, wq_hbm, offset_hbm,
    landed, read_out,
    x_in, scaled, keys, inverse, next_in, gain_in, wk, wv, wq, offset, later_than,
    outgoing, message, gathered,
    x_sem, load_sem,
    b_ssem, b_rsem, m_ssem, m_rsem, ready,
):
    me = lax.axis_index("sp")
    lane = lax.axis_index("tp")
    span, width = x_hbm.shape[0], wk_hbm.shape[1]
    heads = width // HEAD_DIM
    sub = span // n_sp
    rows = span // chunks
    unroll = n_sp <= 16

    upper = me // ((n_sp + 1) // 2)
    early = min(2, n_sp - 1)

    load_gain, load_next, load_offset, load_key, load_query, load_value = [
        pltpu.make_async_copy(hbm, vmem, load_sem.at[n])
        for n, (hbm, vmem) in enumerate(
            [
                (gain_hbm, gain_in),
                (next_hbm, next_in),
                (offset_hbm, offset),
                (wk_hbm, wk),
                (wq_hbm, wq),
                (wv_hbm, wv),
            ]
        )
    ]
    starts = [c * rows for c in range(chunks)]
    x_loads = [
        pltpu.make_async_copy(
            x_hbm.at[pl.ds(starts[c], rows)], x_in.at[pl.ds(starts[c], rows)], x_sem.at[c]
        )
        for c in range(chunks)
    ]
    load_gain.start()
    for load in x_loads:
        load.start()
    load_key.start()
    load_next.start()
    load_offset.start()

    barrier = pltpu.get_barrier_semaphore()

    @pl.loop(1, n_sp)
    def _(step):
        pl.semaphore_signal(
            barrier, inc=1, device_id=(lax.rem(me + step, n_sp), lane), device_id_type=MESH
        )

    @pl.loop(1, n_tp)
    def _(step):
        pl.semaphore_signal(
            barrier, inc=1, device_id=(me, lax.rem(lane + step, n_tp)), device_id_type=MESH
        )

    later_than[...] = jnp.where(
        lax.broadcasted_iota(jnp.int32, (span, span), 0)
        > lax.broadcasted_iota(jnp.int32, (span, span), 1),
        1.0,
        0.0,
    ).astype(jnp.bfloat16)

    load_gain.wait()
    load_query.start()
    load_value.start()
    gain = gain_in[...]
    step_rows = 16 if rows % 16 == 0 else rows

    def scale_rows(c):
        for first in range(starts[c], starts[c] + rows, step_rows):
            scaled[first : first + step_rows, :] = (
                x_in[first : first + step_rows, :].astype(jnp.float32) * gain
            ).astype(jnp.bfloat16)

    def project(c, weight):
        return jnp.dot(
            scaled[starts[c] : starts[c] + rows, :],
            weight[...],
            preferred_element_type=jnp.float32,
        )

    def factor_of(c):
        return jnp.concatenate(
            [
                inverse_rms(x_in[first : first + step_rows, :].astype(jnp.float32))
                for first in range(starts[c], starts[c] + rows, step_rows)
            ],
            axis=0,
        )

    def partner(order):
        return order + jnp.where(order >= me, 1, 0)

    def block_copy(part, order):
        to = partner(order)
        return pltpu.make_async_remote_copy(
            src_ref=outgoing.at[part * n_sp + to], dst_ref=landed.at[part * n_sp + me],
            send_sem=b_ssem, recv_sem=b_rsem,
            device_id=(to, lane), device_id_type=MESH,
        )

    def greet():
        pl.semaphore_wait(barrier, n_sp + n_tp - 2)

        @pl.loop(1, n_tp)
        def _(step):
            pl.semaphore_signal(
                ready, inc=1, device_id=(me, lax.rem(lane + step, n_tp)), device_id_type=MESH
            )

    for load in x_loads:
        load.wait()
    load_key.wait()
    wide_keys = []
    for c in range(chunks):
        scale_rows(c)
        wide_keys.append(project(c, wk))
    factor = jnp.concatenate([factor_of(c) for c in range(chunks)], axis=0)
    wide_keys = jnp.concatenate(wide_keys, axis=0) * factor
    inverse[...] = jnp.broadcast_to(factor, inverse.shape)
    keys[...] = wide_keys.astype(jnp.bfloat16)
    pack_blocks(wide_keys, outgoing, 0, heads, sub)

    @pl.when(upper == 1)
    def _():
        greet()
        block_copy(0, 0).start()

    load_next.wait()
    load_offset.wait()
    load_query.wait()
    load_value.wait()
    next_row = next_in[...].astype(jnp.float32)
    next_row = jnp.concatenate([next_row[n : n + 1] for n in range(next_row.shape[0])], axis=1)
    next_scaled = jnp.broadcast_to((next_row * gain).astype(jnp.bfloat16), (16, x_hbm.shape[1]))
    query = jnp.dot(next_scaled, wq[...], preferred_element_type=jnp.float32)
    query = query * inverse_rms(next_row)
    row_ids = lax.broadcasted_iota(jnp.int32, query.shape, 0)
    head_ids = lax.broadcasted_iota(jnp.int32, query.shape, 1) // HEAD_DIM
    query = jnp.where(row_ids == head_ids, query, 0.0).astype(jnp.bfloat16)
    wide_values = []
    for c in range(0):
        wide_values.append(project(c, wv))

    logits = lax.dot_general(
        query, keys[...], (((1,), (1,)), ((), ())), preferred_element_type=jnp.float32
    )[:heads]
    for c in range(0, chunks):
        wide_values.append(project(c, wv))
    logits = logits * HEAD_DIM ** (-0.5) + offset[...]
    tail = jnp.log1p(jnp.exp(-jnp.abs(logits)))
    log_breaks = -jnp.maximum(logits, 0.0) - tail
    inner = fold_parts(
        jnp.dot(split_parts(log_breaks, 3), later_than[...], preferred_element_type=jnp.float32),
        heads,
    )
    block_total = jnp.sum(log_breaks, axis=1, keepdims=True)
    weights = jnp.exp(jnp.minimum(logits, 0.0) - tail + inner)
    scale = inverse[...]
    wide_values = jnp.concatenate(wide_values, axis=0) * jnp.concatenate([scale] * heads, axis=1)
    read = fold_parts(
        jnp.dot(
            split_parts(weights, 2),
            wide_values.astype(jnp.bfloat16),
            preferred_element_type=jnp.float32,
        ),
        heads,
    )
    high = block_total.astype(jnp.bfloat16).astype(jnp.float32)
    low = block_total - high
    half = lax.broadcasted_iota(jnp.int32, (heads, HEAD_DIM), 1) < HEAD_DIM // 2
    message[...] = jnp.concatenate(
        [
            read[head : head + 1, head * HEAD_DIM : (head + 1) * HEAD_DIM]
            for head in range(heads)
        ]
        + [jnp.where(half, high, low)],
        axis=0,
    ).astype(jnp.bfloat16)
    gathered[me * n_tp + lane] = message[...]
    pack_blocks(wide_values, outgoing, n_sp, heads, sub)

    @pl.when(upper == 0)
    def _():
        greet()
        for order in range(early):
            block_copy(0, order).start()
            block_copy(1, order).start()

    pl.semaphore_wait(ready, n_tp - 1)

    def message_copy(to, step):
        return pltpu.make_async_remote_copy(
            src_ref=message, dst_ref=gathered.at[me * n_tp + lane],
            send_sem=m_ssem, recv_sem=m_rsem,
            device_id=(to, lax.rem(lane + step, n_tp)), device_id_type=MESH,
        )

    @pl.loop(0, n_sp - 1, unroll=unroll)
    def _(order):
        for step in range(n_tp):
            message_copy(partner(order), step).start()

    for step in range(1, n_tp):
        message_copy(me, step).start()

    @pl.when(upper == 1)
    def _():
        block_copy(1, 0).start()
        for order in range(1, early):
            block_copy(0, order).start()
            block_copy(1, order).start()

    @pl.loop(early, n_sp - 1, unroll=unroll)
    def _(order):
        block_copy(0, order).start()
        block_copy(1, order).start()

    landed[me] = outgoing[me]
    landed[n_sp + me] = outgoing[n_sp + me]

    everyone = gathered.at[pl.ds(0, n_sp * n_tp - 1)]
    pltpu.make_async_copy(everyone, everyone, m_rsem).wait()

    def add_block(step, carry):
        block = [gathered[(n_sp - 1 - step) * n_tp + part].astype(jnp.float32) for part in range(n_tp)]
        fresh = []
        for (total, carried), piece in zip(carry, block):
            total = total + jnp.exp(carried) * piece[:heads]
            halves = piece[heads:]
            fresh.append((total, carried + halves + pltpu.roll(halves, HEAD_DIM // 2, 1)))
        return tuple(fresh)

    zero = jnp.zeros((heads, HEAD_DIM), jnp.float32)
    totals = lax.fori_loop(0, n_sp, add_block, ((zero, zero),) * n_tp, unroll=unroll)
    read_out[...] = jnp.concatenate([total for total, _ in totals], axis=0).astype(jnp.bfloat16)

    pltpu.make_async_copy(everyone, everyone, m_ssem).wait()
    others = landed.at[pl.ds(0, 2 * n_sp - 2)]
    pltpu.make_async_copy(others, others, b_ssem).wait()
    pltpu.make_async_copy(others, others, b_rsem).wait()


def finish(landed, read_in, k_out, v_out, read_out):
    sub, n_sp, width = k_out.shape
    heads = width // HEAD_DIM
    for part, out in enumerate((k_out, v_out)):
        for head in range(heads):
            piece = landed[part * n_sp : (part + 1) * n_sp].astype(jnp.float32)[:, head * sub : (head + 1) * sub, :]
            out[:, :, head * HEAD_DIM : (head + 1) * HEAD_DIM] = jnp.swapaxes(
                piece, 0, 1
            ).astype(jnp.bfloat16)
    read_out[...] = read_in[...]


def shards(prompt_input, next_input, norm_gain, w_key, w_value, w_query, key_offset):
    span, depth = prompt_input.shape
    width = w_key.shape[1]
    heads = width // HEAD_DIM
    n_sp, n_tp = lax.axis_size("sp"), lax.axis_size("tp")
    sub = span // n_sp
    chunks = 2 if n_sp % 2 == 0 and span % 32 == 0 else 1
    wide, narrow = jnp.float32, jnp.bfloat16
    blocks = (2 * n_sp, heads * sub, HEAD_DIM)
    sems = pltpu.SemaphoreType.DMA
    landed = pl.pallas_call(
        functools.partial(kernel, n_sp, n_tp, chunks),
        out_shape=(
            jax.ShapeDtypeStruct(blocks, narrow),
            jax.ShapeDtypeStruct((n_tp * heads, HEAD_DIM), narrow),
        ),
        in_specs=[pl.BlockSpec(memory_space=pltpu.HBM)] * 7,
        out_specs=(pl.BlockSpec(memory_space=pltpu.VMEM),) * 2,
        scratch_shapes=[
            pltpu.VMEM((span, depth), narrow),
            pltpu.VMEM((span, depth), narrow),
            pltpu.VMEM((span, width), narrow),
            pltpu.VMEM((span, HEAD_DIM), wide),
            pltpu.VMEM((depth // HEAD_DIM, HEAD_DIM), narrow),
            pltpu.VMEM((1, depth), wide),
            pltpu.VMEM((depth, width), narrow),
            pltpu.VMEM((depth, width), narrow),
            pltpu.VMEM((depth, width), narrow),
            pltpu.VMEM((heads, span), wide),
            pltpu.VMEM((span, span), narrow),
            pltpu.VMEM(blocks, narrow),
            pltpu.VMEM((2 * heads, HEAD_DIM), narrow),
            pltpu.VMEM((n_sp * n_tp, 2 * heads, HEAD_DIM), narrow),
            sems((chunks,)),
            sems((6,)),
            sems,
            sems,
            sems,
            sems,
            pltpu.SemaphoreType.REGULAR,
        ],
        compiler_params=pltpu.CompilerParams(
            collective_id=0, has_side_effects=True, vmem_limit_bytes=16 * 2**20
        ),
        name="prefill",
    )(
        *[
            pltpu.with_memory_space_constraint(operand, pltpu.HBM)
            for operand in (
                prompt_input,
                next_input.reshape(-1, HEAD_DIM),
                norm_gain[None],
                w_key,
                w_value,
                w_query,
                key_offset.T,
            )
        ]
    )
    slotted = jax.ShapeDtypeStruct((sub, n_sp, width), narrow)
    key_cache, value_cache, reading = pl.pallas_call(
        finish,
        out_shape=(slotted, slotted, jax.ShapeDtypeStruct((n_tp * heads, HEAD_DIM), narrow)),
        in_specs=[pl.BlockSpec(memory_space=pltpu.VMEM)] * 2,
        out_specs=(pl.BlockSpec(memory_space=pltpu.VMEM),) * 3,
        compiler_params=pltpu.CompilerParams(vmem_limit_bytes=16 * 2**20),
        name="finish",
    )(*landed)
    return (
        jnp.swapaxes(key_cache, 0, 1)[None],
        jnp.swapaxes(value_cache, 0, 1)[None],
        reading.reshape(-1),
    )


def solution(mesh):
    placed = (P("sp", None), P(), P(), P(None, "tp"), P(None, "tp"), P(None, "tp"), P("sp", "tp"))
    return jax.shard_map(
        shards,
        mesh=mesh,
        in_specs=placed,
        out_specs=(P("sp", None, None, "tp"), P("sp", None, None, "tp"), P()),
        check_vma=False,
    )
```

```python
import functools

import jax
import jax.numpy as jnp
from jax import lax
from jax.experimental import pallas as pl
from jax.experimental.pallas import tpu as pltpu
from jax.sharding import PartitionSpec as P

HEAD_DIM = 128
MESH = pl.DeviceIdType.MESH


def inverse_rms(wide):
    return lax.rsqrt(jnp.mean(wide * wide, axis=-1, keepdims=True) + 1e-06)


def split_parts(wide, count):
    parts = []
    for _ in range(count):
        part = wide.astype(jnp.bfloat16).astype(jnp.float32)
        parts.append(part)
        wide = wide - part
    return jnp.concatenate(parts, axis=0).astype(jnp.bfloat16)


def fold_parts(rows, heads):
    total = rows[:heads]
    for first in range(heads, rows.shape[0], heads):
        total = total + rows[first : first + heads]
    return total


def pack_blocks(wide, outgoing, first, heads, sub):
    for slot in range(wide.shape[0] // sub):
        outgoing[first + slot] = jnp.concatenate(
            [
                wide[slot * sub : (slot + 1) * sub, head * HEAD_DIM : (head + 1) * HEAD_DIM]
                for head in range(heads)
            ],
            axis=0,
        ).astype(jnp.bfloat16)


def kernel(
    n_sp, n_tp, chunks,
    x_hbm, next_hbm, gain_hbm, wk_hbm, wv_hbm, wq_hbm, offset_hbm,
    landed, read_out,
    x_in, scaled, keys, inverse, next_in, gain_in, wk, wv, wq, offset, later_than,
    outgoing, message, gathered,
    x_sem, load_sem,
    b_ssem, b_rsem, m_ssem, m_rsem, ready,
):
    me = lax.axis_index("sp")
    lane = lax.axis_index("tp")
    span, width = x_hbm.shape[0], wk_hbm.shape[1]
    heads = width // HEAD_DIM
    sub = span // n_sp
    rows = span // chunks
    unroll = n_sp <= 16

    upper = me // ((n_sp + 1) // 2)
    early = min(4, n_sp - 1)

    load_gain, load_next, load_offset, load_key, load_query, load_value = [
        pltpu.make_async_copy(hbm, vmem, load_sem.at[n])
        for n, (hbm, vmem) in enumerate(
            [
                (gain_hbm, gain_in),
                (next_hbm, next_in),
                (offset_hbm, offset),
                (wk_hbm, wk),
                (wq_hbm, wq),
                (wv_hbm, wv),
            ]
        )
    ]
    starts = [c * rows for c in range(chunks)]
    x_loads = [
        pltpu.make_async_copy(
            x_hbm.at[pl.ds(starts[c], rows)], x_in.at[pl.ds(starts[c], rows)], x_sem.at[c]
        )
        for c in range(chunks)
    ]
    load_gain.start()
    for load in x_loads:
        load.start()
    load_key.start()
    load_next.start()
    load_offset.start()

    barrier = pltpu.get_barrier_semaphore()

    @pl.loop(1, n_sp)
    def _(step):
        pl.semaphore_signal(
            barrier, inc=1, device_id=(lax.rem(me + step, n_sp), lane), device_id_type=MESH
        )

    @pl.loop(1, n_tp)
    def _(step):
        pl.semaphore_signal(
            barrier, inc=1, device_id=(me, lax.rem(lane + step, n_tp)), device_id_type=MESH
        )

    load_query.start()
    load_value.start()
    later_than[...] = jnp.where(
        lax.broadcasted_iota(jnp.int32, (span, span), 0)
        > lax.broadcasted_iota(jnp.int32, (span, span), 1),
        1.0,
        0.0,
    ).astype(jnp.bfloat16)

    load_gain.wait()
    gain = gain_in[...]
    step_rows = 16 if rows % 16 == 0 else rows

    depth = x_hbm.shape[1]
    cut = depth // 2 if depth % 512 == 0 else depth

    def norm_rows(c):
        for first in range(c * rows, (c + 1) * rows, step_rows):
            wide = x_in[first : first + step_rows, :].astype(jnp.float32)
            scaled[first : first + step_rows, :] = (wide * gain).astype(jnp.bfloat16)
            squares = wide * wide
            inverse[first : first + step_rows, :] = sum(
                squares[:, lane_group : lane_group + HEAD_DIM]
                for lane_group in range(0, depth, HEAD_DIM)
            )

    def project(rows_in, weight, factor):
        return sum(
            jnp.dot(
                rows_in[:, first : first + cut],
                weight[first : first + cut, :],
                preferred_element_type=jnp.float32,
            )
            * factor
            for first in range(0, depth, cut)
        )

    def partner(order):
        falling = me - order
        falling = falling + jnp.where(falling <= 0, n_sp - 1, 0)
        falling = jnp.where(order == 0, 0, falling)
        ahead = me + order + jnp.where(me == 0, 1, 0)
        ahead = ahead - jnp.where(ahead >= n_sp, n_sp - 1, 0)
        ahead = jnp.where(order == 0, jnp.where(me == 0, 1, 0), ahead)
        return jnp.where(upper == 1, falling, ahead)

    def block_copy(part, order):
        to = partner(order)
        return pltpu.make_async_remote_copy(
            src_ref=outgoing.at[part * n_sp + to], dst_ref=landed.at[part * n_sp + me],
            send_sem=b_ssem, recv_sem=b_rsem,
            device_id=(to, lane), device_id_type=MESH,
        )

    def greet():
        pl.semaphore_wait(barrier, n_sp + n_tp - 2)

        @pl.loop(1, n_tp)
        def _(step):
            pl.semaphore_signal(
                ready, inc=1, device_id=(me, lax.rem(lane + step, n_tp)), device_id_type=MESH
            )

    for c in range(chunks):
        x_loads[c].wait()
        norm_rows(c)
    load_key.wait()
    factor = lax.rsqrt(jnp.sum(inverse[...], axis=1, keepdims=True) * (1.0 / depth) + 1e-06)
    inverse[...] = jnp.broadcast_to(factor, inverse.shape)
    wide_keys = project(scaled[...], wk, factor)
    keys[...] = wide_keys.astype(jnp.bfloat16)
    pack_blocks(wide_keys, outgoing, 0, heads, sub)

    @pl.when(upper == 1)
    def _():
        greet()
        block_copy(0, 0).start()
        if n_sp > 3:
            block_copy(0, me - 1).start()

    load_next.wait()
    load_offset.wait()
    load_query.wait()
    load_value.wait()
    next_row = next_in[...].astype(jnp.float32)
    next_row = jnp.concatenate([next_row[n : n + 1] for n in range(next_row.shape[0])], axis=1)
    next_scaled = jnp.broadcast_to((next_row * gain).astype(jnp.bfloat16), (16, x_hbm.shape[1]))
    query = project(next_scaled, wq, inverse_rms(next_row))
    row_ids = lax.broadcasted_iota(jnp.int32, query.shape, 0)
    head_ids = lax.broadcasted_iota(jnp.int32, query.shape, 1) // HEAD_DIM
    query = jnp.where(row_ids == head_ids, query, 0.0).astype(jnp.bfloat16)
    middle = span // 2 if span % 32 == 0 else span
    factor = jnp.concatenate([inverse[...]] * heads, axis=1)
    wide_values = [project(scaled[:middle, :], wv, factor[:middle])]
    logits = lax.dot_general(
        query, keys[...], (((1,), (1,)), ((), ())), preferred_element_type=jnp.float32
    )[:heads]
    if middle < span:
        wide_values.append(project(scaled[middle:, :], wv, factor[middle:]))
    logits = logits * HEAD_DIM ** (-0.5) + offset[...]
    tail = jnp.log1p(jnp.exp(-jnp.abs(logits)))
    log_breaks = -jnp.maximum(logits, 0.0) - tail
    inner = fold_parts(
        jnp.dot(split_parts(log_breaks, 3), later_than[...], preferred_element_type=jnp.float32),
        heads,
    )
    block_total = jnp.sum(log_breaks, axis=1, keepdims=True)
    weights = jnp.exp(jnp.minimum(logits, 0.0) - tail + inner)
    wide_values = jnp.concatenate(wide_values, axis=0)
    read = fold_parts(
        jnp.dot(
            split_parts(weights, 2),
            wide_values.astype(jnp.bfloat16),
            preferred_element_type=jnp.float32,
        ),
        heads,
    )
    high = block_total.astype(jnp.bfloat16).astype(jnp.float32)
    low = block_total - high
    half = lax.broadcasted_iota(jnp.int32, (heads, HEAD_DIM), 1) < HEAD_DIM // 2
    message[...] = jnp.concatenate(
        [
            read[head : head + 1, head * HEAD_DIM : (head + 1) * HEAD_DIM]
            for head in range(heads)
        ]
        + [jnp.where(half, high, low)],
        axis=0,
    ).astype(jnp.bfloat16)
    gathered[me * n_tp + lane] = message[...]
    pack_blocks(wide_values, outgoing, n_sp, heads, sub)

    @pl.when(upper == 0)
    def _():
        greet()
        for order in range(early):
            block_copy(0, order).start()
            block_copy(1, order).start()

    @pl.when(upper == 1)
    def _():
        block_copy(1, 0).start()

    pl.semaphore_wait(ready, n_tp - 1)

    def message_copy(to, step):
        return pltpu.make_async_remote_copy(
            src_ref=message, dst_ref=gathered.at[me * n_tp + lane],
            send_sem=m_ssem, recv_sem=m_rsem,
            device_id=(to, lax.rem(lane + step, n_tp)), device_id_type=MESH,
        )

    @pl.loop(0, n_sp - 1, unroll=unroll)
    def _(order):
        for step in range(n_tp):
            message_copy(partner(order), step).start()

    for step in range(1, n_tp):
        message_copy(me, step).start()

    sent = early * (1 - upper) + upper

    @pl.loop(sent, n_sp - 1)
    def _(order):
        @pl.when((upper == 0) | (order != me - 1) | (n_sp <= 3))
        def _():
            block_copy(0, order).start()

        block_copy(1, order).start()

    landed[me] = outgoing[me]
    landed[n_sp + me] = outgoing[n_sp + me]

    everyone = gathered.at[pl.ds(0, n_sp * n_tp - 1)]
    pltpu.make_async_copy(everyone, everyone, m_rsem).wait()

    def add_block(step, carry):
        block = [gathered[(n_sp - 1 - step) * n_tp + part].astype(jnp.float32) for part in range(n_tp)]
        fresh = []
        for (total, carried), piece in zip(carry, block):
            total = total + jnp.exp(carried) * piece[:heads]
            halves = piece[heads:]
            fresh.append((total, carried + halves + pltpu.roll(halves, HEAD_DIM // 2, 1)))
        return tuple(fresh)

    zero = jnp.zeros((heads, HEAD_DIM), jnp.float32)
    totals = lax.fori_loop(0, n_sp, add_block, ((zero, zero),) * n_tp, unroll=unroll)
    read_out[...] = jnp.concatenate([total for total, _ in totals], axis=0).astype(jnp.bfloat16)

    pltpu.make_async_copy(everyone, everyone, m_ssem).wait()
    others = landed.at[pl.ds(0, 2 * n_sp - 2)]
    pltpu.make_async_copy(others, others, b_ssem).wait()
    pltpu.make_async_copy(others, others, b_rsem).wait()


def finish(landed, read_in, k_out, v_out, read_out):
    sub, n_sp, width = k_out.shape
    heads = width // HEAD_DIM
    for part, out in enumerate((k_out, v_out)):
        for head in range(heads):
            piece = landed[part * n_sp : (part + 1) * n_sp].astype(jnp.float32)[:, head * sub : (head + 1) * sub, :]
            out[:, :, head * HEAD_DIM : (head + 1) * HEAD_DIM] = jnp.swapaxes(
                piece, 0, 1
            ).astype(jnp.bfloat16)
    read_out[...] = read_in[...]


def shards(prompt_input, next_input, norm_gain, w_key, w_value, w_query, key_offset):
    span, depth = prompt_input.shape
    width = w_key.shape[1]
    heads = width // HEAD_DIM
    n_sp, n_tp = lax.axis_size("sp"), lax.axis_size("tp")
    sub = span // n_sp
    chunks = 3 if span % 48 == 0 else 1
    wide, narrow = jnp.float32, jnp.bfloat16
    blocks = (2 * n_sp, heads * sub, HEAD_DIM)
    sems = pltpu.SemaphoreType.DMA
    landed = pl.pallas_call(
        functools.partial(kernel, n_sp, n_tp, chunks),
        out_shape=(
            jax.ShapeDtypeStruct(blocks, narrow),
            jax.ShapeDtypeStruct((n_tp * heads, HEAD_DIM), narrow),
        ),
        in_specs=[pl.BlockSpec(memory_space=pltpu.HBM)] * 7,
        out_specs=(pl.BlockSpec(memory_space=pltpu.VMEM),) * 2,
        scratch_shapes=[
            pltpu.VMEM((span, depth), narrow),
            pltpu.VMEM((span, depth), narrow),
            pltpu.VMEM((span, width), narrow),
            pltpu.VMEM((span, HEAD_DIM), wide),
            pltpu.VMEM((depth // HEAD_DIM, HEAD_DIM), narrow),
            pltpu.VMEM((1, depth), wide),
            pltpu.VMEM((depth, width), narrow),
            pltpu.VMEM((depth, width), narrow),
            pltpu.VMEM((depth, width), narrow),
            pltpu.VMEM((heads, span), wide),
            pltpu.VMEM((span, span), narrow),
            pltpu.VMEM(blocks, narrow),
            pltpu.VMEM((2 * heads, HEAD_DIM), narrow),
            pltpu.VMEM((n_sp * n_tp, 2 * heads, HEAD_DIM), narrow),
            sems((chunks,)),
            sems((6,)),
            sems,
            sems,
            sems,
            sems,
            pltpu.SemaphoreType.REGULAR,
        ],
        compiler_params=pltpu.CompilerParams(
            collective_id=0, has_side_effects=True, vmem_limit_bytes=16 * 2**20
        ),
        name="prefill",
    )(
        *[
            pltpu.with_memory_space_constraint(operand, pltpu.HBM)
            for operand in (
                prompt_input,
                next_input.reshape(-1, HEAD_DIM),
                norm_gain[None],
                w_key,
                w_value,
                w_query,
                key_offset.T,
            )
        ]
    )
    slotted = jax.ShapeDtypeStruct((sub, n_sp, width), narrow)
    key_cache, value_cache, reading = pl.pallas_call(
        finish,
        out_shape=(slotted, slotted, jax.ShapeDtypeStruct((n_tp * heads, HEAD_DIM), narrow)),
        in_specs=[pl.BlockSpec(memory_space=pltpu.VMEM)] * 2,
        out_specs=(pl.BlockSpec(memory_space=pltpu.VMEM),) * 3,
        compiler_params=pltpu.CompilerParams(vmem_limit_bytes=16 * 2**20),
        name="finish",
    )(*landed)
    return (
        jnp.swapaxes(key_cache, 0, 1)[None],
        jnp.swapaxes(value_cache, 0, 1)[None],
        reading.reshape(-1),
    )


def solution(mesh):
    placed = (P("sp", None), P(), P(), P(None, "tp"), P(None, "tp"), P(None, "tp"), P("sp", "tp"))
    return jax.shard_map(
        shards,
        mesh=mesh,
        in_specs=placed,
        out_specs=(P("sp", None, None, "tp"), P("sp", None, None, "tp"), P()),
        check_vma=False,
    )
```

```python
import functools

import jax
import jax.numpy as jnp
from jax import lax
from jax.experimental import pallas as pl
from jax.experimental.pallas import tpu as pltpu
from jax.sharding import PartitionSpec as P

HEAD_DIM = 128
MESH = pl.DeviceIdType.MESH


def inverse_rms(wide):
    return lax.rsqrt(jnp.mean(wide * wide, axis=-1, keepdims=True) + 1e-06)


def split_parts(wide, count):
    parts = []
    for _ in range(count):
        part = wide.astype(jnp.bfloat16).astype(jnp.float32)
        parts.append(part)
        wide = wide - part
    return jnp.concatenate(parts, axis=0).astype(jnp.bfloat16)


def fold_parts(rows, heads):
    total = rows[:heads]
    for first in range(heads, rows.shape[0], heads):
        total = total + rows[first : first + heads]
    return total


def pack_blocks(wide, outgoing, first, heads, sub):
    for slot in range(wide.shape[0] // sub):
        outgoing[first + slot] = jnp.concatenate(
            [
                wide[slot * sub : (slot + 1) * sub, head * HEAD_DIM : (head + 1) * HEAD_DIM]
                for head in range(heads)
            ],
            axis=0,
        ).astype(jnp.bfloat16)


def kernel(
    n_sp, n_tp, chunks,
    x_hbm, next_hbm, gain_hbm, wk_hbm, wv_hbm, wq_hbm, offset_hbm,
    landed, read_out,
    x_in, scaled, keys, inverse, next_in, gain_in, wk, wv, wq, offset, later_than,
    outgoing, message, gathered,
    x_sem, load_sem,
    b_ssem, b_rsem, m_ssem, m_rsem, ready,
):
    me = lax.axis_index("sp")
    lane = lax.axis_index("tp")
    span, width = x_hbm.shape[0], wk_hbm.shape[1]
    heads = width // HEAD_DIM
    sub = span // n_sp
    rows = span // chunks
    unroll = n_sp <= 16

    upper = me // ((n_sp + 1) // 2)
    early = min(3, n_sp - 1)

    load_gain, load_next, load_offset, load_key, load_query, load_value = [
        pltpu.make_async_copy(hbm, vmem, load_sem.at[n])
        for n, (hbm, vmem) in enumerate(
            [
                (gain_hbm, gain_in),
                (next_hbm, next_in),
                (offset_hbm, offset),
                (wk_hbm, wk),
                (wq_hbm, wq),
                (wv_hbm, wv),
            ]
        )
    ]
    starts = [c * rows for c in range(chunks)]
    x_loads = [
        pltpu.make_async_copy(
            x_hbm.at[pl.ds(starts[c], rows)], x_in.at[pl.ds(starts[c], rows)], x_sem.at[c]
        )
        for c in range(chunks)
    ]
    load_gain.start()
    for load in x_loads:
        load.start()
    load_key.start()
    load_next.start()
    load_offset.start()

    barrier = pltpu.get_barrier_semaphore()

    @pl.loop(1, n_sp)
    def _(step):
        pl.semaphore_signal(
            barrier, inc=1, device_id=(lax.rem(me + step, n_sp), lane), device_id_type=MESH
        )

    @pl.loop(1, n_tp)
    def _(step):
        pl.semaphore_signal(
            barrier, inc=1, device_id=(me, lax.rem(lane + step, n_tp)), device_id_type=MESH
        )

    load_query.start()
    load_value.start()
    later_than[...] = jnp.where(
        lax.broadcasted_iota(jnp.int32, (span, span), 0)
        > lax.broadcasted_iota(jnp.int32, (span, span), 1),
        1.0,
        0.0,
    ).astype(jnp.bfloat16)

    load_gain.wait()
    gain = gain_in[...]
    step_rows = 16 if rows % 16 == 0 else rows

    depth = x_hbm.shape[1]
    cut = depth // 2 if depth % 512 == 0 else depth

    def norm_rows(c):
        for first in range(c * rows, (c + 1) * rows, step_rows):
            wide = x_in[first : first + step_rows, :].astype(jnp.float32)
            scaled[first : first + step_rows, :] = (wide * gain).astype(jnp.bfloat16)
            squares = wide * wide
            inverse[first : first + step_rows, :] = sum(
                squares[:, lane_group : lane_group + HEAD_DIM]
                for lane_group in range(0, depth, HEAD_DIM)
            )

    def project(rows_in, weight, factor):
        return sum(
            jnp.dot(
                rows_in[:, first : first + cut],
                weight[first : first + cut, :],
                preferred_element_type=jnp.float32,
            )
            * factor
            for first in range(0, depth, cut)
        )

    def partner(order):
        falling = me - order
        falling = falling + jnp.where(falling <= 0, n_sp - 1, 0)
        falling = jnp.where(order == 0, 0, falling)
        second = me - order + 1
        second = second + jnp.where(second <= 1, n_sp - 2, 0)
        second = jnp.where(order <= 1, order, second)
        falling = jnp.where(me >= n_sp - 2, falling, second)
        ahead = me + order + jnp.where(me == 0, 1, 0)
        ahead = ahead - jnp.where(ahead >= n_sp, n_sp - 1, 0)
        ahead = jnp.where(order == 0, jnp.where(me == 0, 1, 0), ahead)
        return jnp.where(upper == 1, falling, ahead)

    def block_copy(part, order):
        to = partner(order)
        return pltpu.make_async_remote_copy(
            src_ref=outgoing.at[part * n_sp + to], dst_ref=landed.at[part * n_sp + me],
            send_sem=b_ssem, recv_sem=b_rsem,
            device_id=(to, lane), device_id_type=MESH,
        )

    def greet():
        pl.semaphore_wait(barrier, n_sp + n_tp - 2)

        @pl.loop(1, n_tp)
        def _(step):
            pl.semaphore_signal(
                ready, inc=1, device_id=(me, lax.rem(lane + step, n_tp)), device_id_type=MESH
            )

    for c in range(chunks):
        x_loads[c].wait()
        norm_rows(c)
    load_key.wait()
    factor = lax.rsqrt(jnp.sum(inverse[...], axis=1, keepdims=True) * (1.0 / depth) + 1e-06)
    inverse[...] = jnp.broadcast_to(factor, inverse.shape)
    wide_keys = project(scaled[...], wk, factor)
    keys[...] = wide_keys.astype(jnp.bfloat16)
    pack_blocks(wide_keys, outgoing, 0, heads, sub)

    @pl.when(upper == 1)
    def _():
        greet()
        block_copy(0, 0).start()
        if n_sp > 3:
            block_copy(0, jnp.where(me >= n_sp - 2, me - 1, 1)).start()

    load_next.wait()
    load_offset.wait()
    load_query.wait()
    load_value.wait()
    next_row = next_in[...].astype(jnp.float32)
    next_row = jnp.concatenate([next_row[n : n + 1] for n in range(next_row.shape[0])], axis=1)
    next_scaled = jnp.broadcast_to((next_row * gain).astype(jnp.bfloat16), (16, x_hbm.shape[1]))
    query = project(next_scaled, wq, inverse_rms(next_row))
    row_ids = lax.broadcasted_iota(jnp.int32, query.shape, 0)
    head_ids = lax.broadcasted_iota(jnp.int32, query.shape, 1) // HEAD_DIM
    query = jnp.where(row_ids == head_ids, query, 0.0).astype(jnp.bfloat16)
    middle = span // 2 if span % 32 == 0 else span
    factor = jnp.concatenate([inverse[...]] * heads, axis=1)
    wide_values = [project(scaled[:middle, :], wv, factor[:middle])]
    logits = lax.dot_general(
        query, keys[...], (((1,), (1,)), ((), ())), preferred_element_type=jnp.float32
    )[:heads]
    if middle < span:
        wide_values.append(project(scaled[middle:, :], wv, factor[middle:]))
    logits = logits * HEAD_DIM ** (-0.5) + offset[...]
    tail = jnp.log1p(jnp.exp(-jnp.abs(logits)))
    log_breaks = -jnp.maximum(logits, 0.0) - tail
    inner = fold_parts(
        jnp.dot(split_parts(log_breaks, 3), later_than[...], preferred_element_type=jnp.float32),
        heads,
    )
    block_total = jnp.sum(log_breaks, axis=1, keepdims=True)
    weights = jnp.exp(jnp.minimum(logits, 0.0) - tail + inner)
    wide_values = jnp.concatenate(wide_values, axis=0)
    read = fold_parts(
        jnp.dot(
            split_parts(weights, 2),
            wide_values.astype(jnp.bfloat16),
            preferred_element_type=jnp.float32,
        ),
        heads,
    )
    high = block_total.astype(jnp.bfloat16).astype(jnp.float32)
    low = block_total - high
    half = lax.broadcasted_iota(jnp.int32, (heads, HEAD_DIM), 1) < HEAD_DIM // 2
    message[...] = jnp.concatenate(
        [
            read[head : head + 1, head * HEAD_DIM : (head + 1) * HEAD_DIM]
            for head in range(heads)
        ]
        + [jnp.where(half, high, low)],
        axis=0,
    ).astype(jnp.bfloat16)
    gathered[me * n_tp + lane] = message[...]
    pack_blocks(wide_values, outgoing, n_sp, heads, sub)

    @pl.when(upper == 0)
    def _():
        greet()
        block_copy(0, 0).start()
        for order in range(1, early):
            block_copy(0, order).start()
            block_copy(1, order).start()

    @pl.when(upper == 1)
    def _():
        block_copy(1, 0).start()

    pl.semaphore_wait(ready, n_tp - 1)

    def message_copy(to, step):
        return pltpu.make_async_remote_copy(
            src_ref=message, dst_ref=gathered.at[me * n_tp + lane],
            send_sem=m_ssem, recv_sem=m_rsem,
            device_id=(to, lax.rem(lane + step, n_tp)), device_id_type=MESH,
        )

    @pl.loop(0, n_sp - 1, unroll=unroll)
    def _(order):
        for step in range(n_tp):
            message_copy(partner(order), step).start()

    for step in range(1, n_tp):
        message_copy(me, step).start()

    @pl.when(upper == 0)
    def _():
        block_copy(1, 0).start()

    sent = early * (1 - upper) + upper

    @pl.loop(sent, n_sp - 1)
    def _(order):
        @pl.when((upper == 0) | (order != jnp.where(me >= n_sp - 2, me - 1, 1)) | (n_sp <= 3))
        def _():
            block_copy(0, order).start()

        block_copy(1, order).start()

    landed[me] = outgoing[me]
    landed[n_sp + me] = outgoing[n_sp + me]

    everyone = gathered.at[pl.ds(0, n_sp * n_tp - 1)]
    pltpu.make_async_copy(everyone, everyone, m_rsem).wait()

    def add_block(step, carry):
        block = [gathered[(n_sp - 1 - step) * n_tp + part].astype(jnp.float32) for part in range(n_tp)]
        fresh = []
        for (total, carried), piece in zip(carry, block):
            total = total + jnp.exp(carried) * piece[:heads]
            halves = piece[heads:]
            fresh.append((total, carried + halves + pltpu.roll(halves, HEAD_DIM // 2, 1)))
        return tuple(fresh)

    zero = jnp.zeros((heads, HEAD_DIM), jnp.float32)
    totals = lax.fori_loop(0, n_sp, add_block, ((zero, zero),) * n_tp, unroll=unroll)
    read_out[...] = jnp.concatenate([total for total, _ in totals], axis=0).astype(jnp.bfloat16)

    pltpu.make_async_copy(everyone, everyone, m_ssem).wait()
    others = landed.at[pl.ds(0, 2 * n_sp - 2)]
    pltpu.make_async_copy(others, others, b_ssem).wait()
    pltpu.make_async_copy(others, others, b_rsem).wait()


def finish(landed, read_in, k_out, v_out, read_out):
    sub, n_sp, width = k_out.shape
    heads = width // HEAD_DIM
    for part, out in enumerate((k_out, v_out)):
        for head in range(heads):
            piece = landed[part * n_sp : (part + 1) * n_sp].astype(jnp.float32)[:, head * sub : (head + 1) * sub, :]
            out[:, :, head * HEAD_DIM : (head + 1) * HEAD_DIM] = jnp.swapaxes(
                piece, 0, 1
            ).astype(jnp.bfloat16)
    read_out[...] = read_in[...]


def shards(prompt_input, next_input, norm_gain, w_key, w_value, w_query, key_offset):
    span, depth = prompt_input.shape
    width = w_key.shape[1]
    heads = width // HEAD_DIM
    n_sp, n_tp = lax.axis_size("sp"), lax.axis_size("tp")
    sub = span // n_sp
    chunks = 3 if span % 48 == 0 else 1
    wide, narrow = jnp.float32, jnp.bfloat16
    blocks = (2 * n_sp, heads * sub, HEAD_DIM)
    sems = pltpu.SemaphoreType.DMA
    landed = pl.pallas_call(
        functools.partial(kernel, n_sp, n_tp, chunks),
        out_shape=(
            jax.ShapeDtypeStruct(blocks, narrow),
            jax.ShapeDtypeStruct((n_tp * heads, HEAD_DIM), narrow),
        ),
        in_specs=[pl.BlockSpec(memory_space=pltpu.HBM)] * 7,
        out_specs=(pl.BlockSpec(memory_space=pltpu.VMEM),) * 2,
        scratch_shapes=[
            pltpu.VMEM((span, depth), narrow),
            pltpu.VMEM((span, depth), narrow),
            pltpu.VMEM((span, width), narrow),
            pltpu.VMEM((span, HEAD_DIM), wide),
            pltpu.VMEM((depth // HEAD_DIM, HEAD_DIM), narrow),
            pltpu.VMEM((1, depth), wide),
            pltpu.VMEM((depth, width), narrow),
            pltpu.VMEM((depth, width), narrow),
            pltpu.VMEM((depth, width), narrow),
            pltpu.VMEM((heads, span), wide),
            pltpu.VMEM((span, span), narrow),
            pltpu.VMEM(blocks, narrow),
            pltpu.VMEM((2 * heads, HEAD_DIM), narrow),
            pltpu.VMEM((n_sp * n_tp, 2 * heads, HEAD_DIM), narrow),
            sems((chunks,)),
            sems((6,)),
            sems,
            sems,
            sems,
            sems,
            pltpu.SemaphoreType.REGULAR,
        ],
        compiler_params=pltpu.CompilerParams(
            collective_id=0, has_side_effects=True, vmem_limit_bytes=16 * 2**20
        ),
        name="prefill",
    )(
        *[
            pltpu.with_memory_space_constraint(operand, pltpu.HBM)
            for operand in (
                prompt_input,
                next_input.reshape(-1, HEAD_DIM),
                norm_gain[None],
                w_key,
                w_value,
                w_query,
                key_offset.T,
            )
        ]
    )
    slotted = jax.ShapeDtypeStruct((sub, n_sp, width), narrow)
    key_cache, value_cache, reading = pl.pallas_call(
        finish,
        out_shape=(slotted, slotted, jax.ShapeDtypeStruct((n_tp * heads, HEAD_DIM), narrow)),
        in_specs=[pl.BlockSpec(memory_space=pltpu.VMEM)] * 2,
        out_specs=(pl.BlockSpec(memory_space=pltpu.VMEM),) * 3,
        compiler_params=pltpu.CompilerParams(vmem_limit_bytes=16 * 2**20),
        name="finish",
    )(*landed)
    return (
        jnp.swapaxes(key_cache, 0, 1)[None],
        jnp.swapaxes(value_cache, 0, 1)[None],
        reading.reshape(-1),
    )


def solution(mesh):
    placed = (P("sp", None), P(), P(), P(None, "tp"), P(None, "tp"), P(None, "tp"), P("sp", "tp"))
    return jax.shard_map(
        shards,
        mesh=mesh,
        in_specs=placed,
        out_specs=(P("sp", None, None, "tp"), P("sp", None, None, "tp"), P()),
        check_vma=False,
    )
```
